32 devices in a mesh: sp: 8 (over z, x), dp: 4 (over y, core).
Axes of the slice: x: 2, y: 2, z: 4, core: 2. Of those that a mesh axis runs over, the one named last changes fastest.
Arguments:
- stream_in: bfloat16 [4, 1024, 4096], P('dp', 'sp'), may hold values from -6 to 6
- query_rows: bfloat16 [4, 1024, 2048], P('dp', 'sp'), may hold values from -310 to 310
- key_rows: bfloat16 [4, 1024, 2048], P('dp', 'sp'), may hold values from -12 to 12
- value_rows: bfloat16 [4, 1024, 2048], P('dp', 'sp'), may hold values from -6 to 6
- log_forget: float32 [4, 16, 1024], P('dp', 'sp'), may hold values from -256 to 0, as said below
- out_weight: bfloat16 [2048, 4096], P(None, 'dp'), may hold values from -0.5 to 0.5
- norm_gain: float32 [4096], replicated, may hold values from 0.1 to 1.9
- expert_ids: int32 [4, 1024, 4], P('dp', 'sp'), may hold values from 0 to 31, all different within a row; in each aligned block of 128 rows (0 to 127, 128 to 255, ..., all dimensions but the last counted through in order) at most 20 rows name the same one
- route_weights: float32 [4, 1024, 4], P('dp', 'sp'), may hold values from 0.1 to 1
- gate_weight: bfloat16 [32, 4096, 512], P(('sp', 'dp')), may hold values from -0.25 to 0.25
- up_weight: bfloat16 [32, 4096, 512], P(('sp', 'dp')), may hold values from -0.25 to 0.25
- down_weight: bfloat16 [32, 512, 4096], P(('sp', 'dp')), may hold values from -0.0625 to 0.0625
- final_gain: float32 [4096], replicated, may hold values from 0.1 to 1.9
Outputs:
- layer_out: bfloat16 [4, 1024, 4096], P('dp', 'sp')
The draws below stay inside these ranges and needn't reach their ends.
Inputs may be any that keep to these rules, and one draw needn't show every extreme that they name: `expert_ids`: each row names 4 different experts; in the rows of one device no expert is named more than 20 times. `log_forget`: never rising along positions.
All inputs are finite; a program needn't handle non-finite values.
Results may differ from the reference program's by a relative error of at most 0.01.
Values may be sent and summed in bfloat16 or wider, within the bound.
A program may use at most 128 MiB of HBM per device.

```python
import math
import jax
import jax.numpy as jnp
import numpy as np
from jax import lax

D = 4096
HEAD_TOTAL = 16
HEAD_DIM = 128
FFE = 512
TOP_K = 4
TOK_DEV = 128
SEQUENCE_COUNT = 4
SEQUENCE_LENGTH = 1024
EXPERTS = 32
CAP = 20


def drawn_pair(key):
    query_key, key_key = jax.random.split(jax.random.fold_in(key, 7), 2)
    row_width = HEAD_TOTAL * HEAD_DIM
    queries = jax.random.truncated_normal(query_key, -4.0, 4.0, (SEQUENCE_COUNT, SEQUENCE_LENGTH, row_width), jnp.float32)
    keys_all = jax.random.truncated_normal(key_key, -4.0, 4.0, (SEQUENCE_COUNT, SEQUENCE_LENGTH, row_width), jnp.float32)
    return (queries, keys_all)


def draw_query_rows(key, part):
    return drawn_pair(key)[0].astype(jnp.bfloat16)


def draw_key_rows(key, part):
    return drawn_pair(key)[1].astype(jnp.bfloat16)


def draw_log_forget(key, part):
    perm_key, block_key, rough_key, spike_random_key, loss_key = jax.random.split(jax.random.fold_in(key, 11), 5)
    fast_share = 0.5
    head_order = jax.random.permutation(perm_key, HEAD_TOTAL)
    quick_decay_flag = (head_order < int(HEAD_TOTAL * fast_share))[None, :, None]
    decay_rate = jnp.where(quick_decay_flag, 1.0 / 40.0, 0.5 / SEQUENCE_LENGTH)
    block_count = SEQUENCE_LENGTH // TOK_DEV
    block_multiplier = jnp.exp(jax.random.uniform(block_key, (SEQUENCE_COUNT, HEAD_TOTAL, block_count), jnp.float32, -0.7, 0.7))
    block_multiplier = jnp.repeat(block_multiplier, TOK_DEV, axis=2)
    jitter_level = jax.random.uniform(rough_key, (SEQUENCE_COUNT, HEAD_TOTAL, SEQUENCE_LENGTH), jnp.float32, 0.5, 2.0)
    spike_positions = jax.random.randint(spike_random_key, (SEQUENCE_COUNT, HEAD_TOTAL, 3), 0, SEQUENCE_LENGTH)
    decay_amounts = jax.random.uniform(loss_key, (SEQUENCE_COUNT, HEAD_TOTAL, 3), jnp.float32, 0.22, 0.69)
    token_positions = jnp.arange(SEQUENCE_LENGTH)
    spike_events = jnp.sum(jnp.where(token_positions[None, None, None, :] == spike_positions[..., None], decay_amounts[..., None], 0.0), axis=2)
    forget_steps = -decay_rate * block_multiplier * jitter_level - jnp.where(quick_decay_flag, 0.0, spike_events)
    return jnp.cumsum(forget_steps, axis=-1)


def block_levels(key, dims, pieces, smallest, top_value):
    factor_of = 1.0
    for dim, shards_of in pieces:
        steps = jax.random.uniform(jax.random.fold_in(jax.random.fold_in(key, 6), dim), (shards_of,), jnp.float32, smallest / len(pieces), top_value / len(pieces))
        factor_of = factor_of * jnp.repeat(jnp.exp(steps), dims[dim] // shards_of).reshape((-1,) + (1,) * (len(dims) - 1 - dim))
    return factor_of


def deal_out(key, own, number, rows, count, top, limit, lean):
    ranking = jax.random.permutation(key, count)
    heavy_load, common = load_shares(count, rows * top, limit, lean, True), load_shares(count, rows * top, limit, lean, False)
    places = jnp.arange(count)

    def named(tallies, turn):
        used = int((tallies > 0).sum())
        fixed = max(1, used // 4)
        passed = fixed + (places - fixed + turn * (used - fixed)) % max(1, count - fixed)
        return jnp.zeros((count,), jnp.int32).at[ranking[jnp.where(places < fixed, places, passed)]].set(jnp.asarray(tallies, jnp.int32))

    tallies = jnp.where(number % 4 == 0, named(heavy_load, number // 4), named(common, number - number // 4 - 1))
    mixed = jax.random.permutation(jax.random.fold_in(own, 3), count)
    source_of, taker = mixed[0:count // 2 * 2:2], mixed[1:count // 2 * 2:2]
    margin = jnp.minimum(tallies[source_of] - 1, limit - tallies[taker]) // 2
    margin = jnp.where((source_of == ranking[0]) | (taker == ranking[0]) | (tallies[taker] == 0), 0, jnp.maximum(margin, 0))
    passed = jax.random.randint(jax.random.fold_in(own, 4), (count // 2,), 0, 1 << 20) % (margin + 1)
    tallies = tallies.at[source_of].add(-passed).at[taker].add(passed)
    members = jnp.searchsorted(jnp.cumsum(tallies), jnp.arange(rows * top), side="right").astype(jnp.int32)
    grid = members.reshape(top, rows).T
    grid = grid[jax.random.permutation(jax.random.fold_in(own, 1), rows)]
    turn = jax.random.randint(jax.random.fold_in(own, 2), (rows, 1), 0, top)
    return jnp.take_along_axis(grid, (jnp.arange(top)[None, :] + turn) % top, axis=1)


def load_shares(number_of, total, limit, lean, full):
    loads = [(1 << 20) // math.isqrt(rank ** lean) + 1 for rank in range(1, number_of + 1)]
    largest = limit if full else min(limit, max(-(-total // number_of), total * loads[0] // sum(loads)))
    least = 1 if total - largest >= number_of - 1 else 0
    holding, surplus = [largest] + [least] * (number_of - 1), total - largest - least * (number_of - 1)
    while surplus > 0:
        candidates = [i for i in range(1, number_of) if holding[i] < largest] or [i for i in range(1, number_of) if holding[i] < limit]
        pool, left = sum([loads[i] for i in candidates]), surplus
        for i in candidates:
            extra = min(limit - holding[i], max(1, left * loads[i] // pool), surplus)
            holding[i] = holding[i] + extra
            surplus = surplus - extra
    return np.array(holding)


def normal_values(stream_key, extent, scale, most, cuts=(), held_as=jnp.bfloat16):
    entries = scale * jax.random.normal(stream_key, extent, jnp.float32)
    if cuts:
        entries = entries * block_levels(stream_key, extent, cuts, -0.22, 0.18)
    return jnp.clip(entries, -most, most).astype(held_as)


def setup_inputs(seed: int = 0) -> dict:
    key_list = jax.random.split(jax.random.key(seed), 14)
    stream_in = normal_values(key_list[0], (SEQUENCE_COUNT, SEQUENCE_LENGTH, D), 1.0, 6.0, ((0, 4), (1, 8)))
    query_rows = draw_query_rows(jax.random.fold_in(key_list[13], 71), 0)
    key_rows = draw_key_rows(jax.random.fold_in(key_list[13], 71), 0)
    value_rows = normal_values(key_list[3], (SEQUENCE_COUNT, SEQUENCE_LENGTH, HEAD_TOTAL * HEAD_DIM), 1.0, 6.0, ((0, 4), (1, 8)))
    log_forget = draw_log_forget(jax.random.fold_in(key_list[13], 71), 0)
    out_weight = normal_values(key_list[5], (HEAD_TOTAL * HEAD_DIM, D), (HEAD_TOTAL * HEAD_DIM // 16) ** -0.5, 0.5, ((1, 4),))
    norm_gain = jnp.clip(1.0 + 0.18 * jax.random.normal(key_list[6], (D,), jnp.float32), 0.1, 1.9)
    expert_ids_keys = jax.random.split(jax.random.fold_in(key_list[7], 1), SEQUENCE_COUNT * SEQUENCE_LENGTH // TOK_DEV)
    expert_ids_turns = jax.random.permutation(jax.random.fold_in(key_list[7], 3), SEQUENCE_COUNT * SEQUENCE_LENGTH // TOK_DEV)
    expert_ids = jax.vmap(lambda own, number: deal_out(jax.random.fold_in(key_list[7], 2), own, number, TOK_DEV, EXPERTS, TOP_K, CAP, 2))(expert_ids_keys, expert_ids_turns).reshape((SEQUENCE_COUNT, SEQUENCE_LENGTH, TOP_K))
    route_weights = jnp.clip(jnp.exp(math.log(1.0) - 2.3025851 * jax.random.uniform(key_list[8], (SEQUENCE_COUNT, SEQUENCE_LENGTH, TOP_K), jnp.float32) ** block_levels(key_list[8], (SEQUENCE_COUNT, SEQUENCE_LENGTH, TOP_K), ((0, 4), (1, 8)), -0.2, 0.2)), 0.1, 1.0)
    gate_weight = normal_values(key_list[9], (EXPERTS, D, FFE), (D // 9) ** -0.5, 0.25, ((0, 32),))
    up_weight = normal_values(key_list[10], (EXPERTS, D, FFE), (D // 9) ** -0.5, 0.25, ((0, 32),))
    down_weight = normal_values(key_list[11], (EXPERTS, FFE, D), (FFE * 16) ** -0.5, 0.0625, ((0, 32),))
    final_gain = jnp.clip(1.0 + 0.18 * jax.random.normal(key_list[12], (D,), jnp.float32), 0.1, 1.9)
    return {"stream_in": stream_in, "query_rows": query_rows, "key_rows": key_rows, "value_rows": value_rows, "log_forget": log_forget, "out_weight": out_weight, "norm_gain": norm_gain, "expert_ids": expert_ids, "route_weights": route_weights, "gate_weight": gate_weight, "up_weight": up_weight, "down_weight": down_weight, "final_gain": final_gain}


resid_scale = 2.0 ** 0.5
clamp_limit = 7.0
gate_slope = 1.702
norm_eps = 1e-05

def normalize_rows(values, gains):
    centre = lax.optimization_barrier(jnp.mean(values, axis=-1, keepdims=True))
    shifted = values - centre
    spread = lax.optimization_barrier(jnp.mean(shifted * shifted, axis=-1, keepdims=True))
    return shifted * lax.rsqrt(spread + norm_eps) * gains.astype(jnp.float32)

def attend_head(query_part, key_part, value_part, gate_sums):
    length = query_part.shape[0]
    block_rows = min(512, length)
    score_scale = query_part.shape[1] ** (-0.5)
    token_positions = jnp.arange(length, dtype=jnp.int32)

    def one_block(offset):
        query_block = lax.dynamic_slice_in_dim(query_part, offset, block_rows, 0)
        scores = lax.dot_general(query_block, key_part, (((1,), (1,)), ((), ())), preferred_element_type=jnp.float32) * score_scale
        own_sums = lax.dynamic_slice_in_dim(gate_sums, offset, block_rows, 0)
        scores = scores + own_sums[:, None] - gate_sums[None, :]
        query_pos = offset + jnp.arange(block_rows, dtype=jnp.int32)
        scores = jnp.where(token_positions[None, :] <= query_pos[:, None], scores, -jnp.inf)
        largest = lax.optimization_barrier(jnp.max(scores, axis=-1, keepdims=True))
        weights = jnp.exp(scores - largest)
        probabilities = (weights / lax.optimization_barrier(jnp.sum(weights, axis=-1, keepdims=True))).astype(jnp.bfloat16)
        return jnp.dot(probabilities, value_part, preferred_element_type=jnp.float32).astype(jnp.bfloat16)
    offsets = jnp.arange(length // block_rows, dtype=jnp.int32) * block_rows
    return lax.map(one_block, offsets).reshape(length, value_part.shape[1])

def expert_rows(inputs, gate_part, up_part, down_part):
    gate_pre = jnp.minimum(jnp.dot(inputs, gate_part, preferred_element_type=jnp.float32), clamp_limit)
    up_pre = jnp.clip(jnp.dot(inputs, up_part, preferred_element_type=jnp.float32), -clamp_limit, clamp_limit)
    activated = ((up_pre + 1.0) * gate_pre * jax.nn.sigmoid(gate_slope * gate_pre)).astype(jnp.bfloat16)
    return jnp.dot(activated, down_part, preferred_element_type=jnp.float32).astype(jnp.bfloat16)

def reference(stream_in, query_rows, key_rows, value_rows, log_forget, out_weight, norm_gain, expert_ids, route_weights, gate_weight, up_weight, down_weight, final_gain):

    def attend_sequence(seq_items):
        seq_query, seq_key, seq_value, seq_gates = seq_items
        length = seq_query.shape[0]
        head_count = seq_gates.shape[0]

        def split_heads(block_data):
            return block_data.reshape(length, head_count, -1).transpose(1, 0, 2)

        def one_head(head_items):
            return attend_head(head_items[0], head_items[1], head_items[2], head_items[3])
        per_head = lax.map(one_head, (split_heads(seq_query), split_heads(seq_key), split_heads(seq_value), seq_gates))
        return per_head.transpose(1, 0, 2).reshape(length, -1)
    attended = lax.map(attend_sequence, (query_rows, key_rows, value_rows, log_forget))
    model_width = stream_in.shape[-1]
    mixed_rows = jnp.dot(attended.reshape(-1, attended.shape[-1]), out_weight, preferred_element_type=jnp.float32).astype(jnp.bfloat16)
    hidden = normalize_rows(resid_scale * stream_in.reshape(-1, model_width).astype(jnp.float32) + mixed_rows.astype(jnp.float32), norm_gain).astype(jnp.bfloat16)
    pair_expert = expert_ids.reshape(-1)
    shares = route_weights / lax.optimization_barrier(jnp.sum(route_weights, axis=-1, keepdims=True))
    pair_share = shares.reshape(-1)
    top_count = expert_ids.shape[-1]
    most_rows = EXPERTS * CAP

    def per_expert(routed_sum, expert_index):
        chosen = pair_expert == expert_index
        picked = jnp.nonzero(chosen, size=most_rows, fill_value=0)[0].astype(jnp.int32)
        is_valid = jnp.arange(most_rows, dtype=jnp.int32) < jnp.sum(chosen.astype(jnp.int32))
        token_index = picked // top_count
        produced = expert_rows(hidden[token_index], gate_weight[expert_index], up_weight[expert_index], down_weight[expert_index])
        factor = jnp.where(is_valid, pair_share[picked], 0.0)
        return (routed_sum.at[token_index].add(produced.astype(jnp.float32) * factor[:, None]), None)
    routed, _ = lax.scan(per_expert, jnp.zeros(hidden.shape, jnp.float32), jnp.arange(EXPERTS, dtype=jnp.int32))
    result = normalize_rows(resid_scale * hidden.astype(jnp.float32) + routed, final_gain).astype(jnp.bfloat16)
    return result.reshape(stream_in.shape)
```

```python
import math

import jax
import jax.numpy as jnp
from jax import lax
from jax.sharding import PartitionSpec as P

resid_scale = 2.0**0.5
clamp_limit = 7.0
gate_slope = 1.702
norm_eps = 1e-05


def normalize_rows(values, gains):
    centre = jnp.mean(values, axis=-1, keepdims=True)
    shifted = values - centre
    spread = jnp.mean(shifted * shifted, axis=-1, keepdims=True)
    return shifted * lax.rsqrt(spread + norm_eps) * gains


def attend_head(query_part, key_part, value_part, gate_sums):
    length = query_part.shape[0]
    block_rows = max(length // 4, min(128, length))
    score_scale = query_part.shape[1] ** (-0.5)
    pieces = []
    for offset in range(0, length, block_rows):
        seen = offset + block_rows
        scores = (
            lax.dot_general(
                query_part[offset:seen],
                key_part[:seen],
                (((1,), (1,)), ((), ())),
                preferred_element_type=jnp.float32,
            )
            * score_scale
        )
        scores = scores + gate_sums[offset:seen, None] - gate_sums[None, :seen]
        query_pos = offset + lax.broadcasted_iota(jnp.int32, scores.shape, 0)
        key_pos = lax.broadcasted_iota(jnp.int32, scores.shape, 1)
        scores = jnp.where(key_pos <= query_pos, scores, -jnp.inf)
        largest = jnp.max(scores, axis=-1, keepdims=True)
        weights = jnp.exp(scores - largest)
        total = jnp.sum(weights, axis=-1, keepdims=True)
        summed = jnp.dot(
            weights.astype(jnp.bfloat16), value_part[:seen], preferred_element_type=jnp.float32
        )
        pieces.append((summed / total).astype(jnp.bfloat16))
    return jnp.concatenate(pieces, axis=0)


def per_device(
    stream_in,
    query_rows,
    key_rows,
    value_rows,
    log_forget,
    out_weight,
    norm_gain,
    expert_ids,
    route_weights,
    gate_weight,
    up_weight,
    down_weight,
    final_gain,
):
    local_heads = log_forget.shape[1]
    sp_count = lax.axis_size("sp")
    token_count, row_width = query_rows.shape[1:]
    head_width = row_width // (local_heads * sp_count)
    full_length = token_count * sp_count
    full_weight = lax.all_gather(out_weight, "dp", axis=1, tiled=True)

    def head_blocks(rows, head_index):
        return jnp.stack(
            [
                rows[0, :, lower : lower + head_width]
                for lower in (
                    (owner * local_heads + head_index) * head_width for owner in range(sp_count)
                )
            ]
        )

    arrived = []
    for head_index in range(local_heads):
        block = jnp.concatenate(
            [head_blocks(rows, head_index) for rows in (query_rows, key_rows, value_rows)], axis=1
        )
        arrived.append(lax.all_to_all(block, "sp", split_axis=0, concat_axis=0, tiled=True))
    returned_heads = []
    for head_index in range(local_heads):
        query_part, key_part, value_part = (
            arrived[head_index][:, part * token_count : (part + 1) * token_count].reshape(
                full_length, head_width
            )
            for part in range(3)
        )
        head_out = attend_head(query_part, key_part, value_part, log_forget[0, head_index])
        returned_heads.append(
            lax.all_to_all(
                head_out.reshape(sp_count, token_count, head_width),
                "sp",
                split_axis=0,
                concat_axis=0,
                tiled=True,
            )
        )
    attended = jnp.concatenate(
        [returned_heads[h][owner] for owner in range(sp_count) for h in range(local_heads)], axis=-1
    )
    mixed_rows = jnp.dot(attended, full_weight, preferred_element_type=jnp.float32).astype(
        jnp.bfloat16
    )
    hidden = normalize_rows(
        resid_scale * stream_in[0].astype(jnp.float32) + mixed_rows.astype(jnp.float32), norm_gain
    ).astype(jnp.bfloat16)
    model_width = hidden.shape[1]
    top_count = expert_ids.shape[2]
    expert_count = sp_count * lax.axis_size("dp")
    capacity = 5 * token_count * top_count // (4 * expert_count)

    folds = 8 // math.gcd(capacity, 8)
    chunk_count = 2
    chunk_width = model_width // chunk_count
    piece_width = chunk_width // folds
    block_rows = folds * capacity

    expert_axis = jnp.arange(expert_count, dtype=jnp.int32)
    named = expert_ids[0][:, :, None] == expert_axis[None, None, :]
    member = jnp.any(named, axis=1)
    earlier = jnp.tril(jnp.ones((token_count, token_count), jnp.float32), -1)
    rank = jnp.dot(
        earlier.astype(jnp.bfloat16),
        member.astype(jnp.bfloat16),
        preferred_element_type=jnp.float32,
    ).astype(jnp.int32)
    shares = route_weights[0] / jnp.sum(route_weights[0], axis=-1, keepdims=True)
    share_of = jnp.sum(jnp.where(named, shares[:, :, None], 0.0), axis=1).T
    share_high = share_of.astype(jnp.bfloat16)
    share_low = (share_of - share_high.astype(jnp.float32)).astype(jnp.bfloat16)
    rank_of = jnp.where(member, rank, -block_rows).T
    code = jnp.concatenate([rank_of + fold * capacity for fold in range(folds)], axis=1)
    code = jnp.where(code < 0, -1, code)
    code = jnp.where(jnp.concatenate([member.T] * folds, axis=1), code, -1)
    match = code[:, None, :] == jnp.arange(block_rows, dtype=jnp.int32)[None, :, None]
    total_rows = expert_count * block_rows
    picks = match.astype(jnp.bfloat16).reshape(total_rows, folds * token_count)

    def weighted(share):
        spread = jnp.concatenate([share] * folds, axis=1)[:, None, :]
        return jnp.where(match, spread, jnp.bfloat16(0)).reshape(total_rows, folds * token_count)

    mix = jnp.concatenate([weighted(share_high), weighted(share_low)], axis=1)

    batches = []
    for chunk in range(chunk_count):
        lower = chunk * chunk_width
        stacked = jnp.concatenate(
            [
                hidden[:, lower + fold * piece_width : lower + (fold + 1) * piece_width]
                for fold in range(folds)
            ],
            axis=0,
        )
        outgoing = jnp.dot(picks, stacked, preferred_element_type=jnp.float32).astype(jnp.bfloat16)
        batches.append(
            lax.all_to_all(
                outgoing.reshape(expert_count, block_rows, piece_width),
                ("sp", "dp"),
                split_axis=0,
                concat_axis=0,
                tiled=True,
            )
        )
    gate_pre = up_pre = 0.0
    for chunk in range(chunk_count):
        lower = chunk * chunk_width
        rows = (
            batches[chunk]
            .reshape(expert_count, folds, capacity, piece_width)
            .transpose(0, 2, 1, 3)
            .reshape(expert_count * capacity, chunk_width)
        )
        upper = lower + chunk_width
        gate_pre += jnp.dot(rows, gate_weight[0, lower:upper], preferred_element_type=jnp.float32)
        up_pre += jnp.dot(rows, up_weight[0, lower:upper], preferred_element_type=jnp.float32)
    gate_pre = jnp.minimum(gate_pre, clamp_limit)
    up_pre = jnp.clip(up_pre, -clamp_limit, clamp_limit)
    activated = ((up_pre + 1.0) * gate_pre * jax.nn.sigmoid(gate_slope * gate_pre)).astype(
        jnp.bfloat16
    )
    returned = []
    for chunk in range(chunk_count):
        lower = chunk * chunk_width
        produced = jnp.dot(
            activated,
            down_weight[0, :, lower : lower + chunk_width],
            preferred_element_type=jnp.float32,
        ).astype(jnp.bfloat16)
        packed = (
            produced.reshape(expert_count, capacity, folds, piece_width)
            .transpose(0, 2, 1, 3)
            .reshape(expert_count, block_rows, piece_width)
        )
        returned.append(
            lax.all_to_all(packed, ("sp", "dp"), split_axis=0, concat_axis=0, tiled=True)
        )
    routed_pieces = []
    for chunk in range(chunk_count):
        back = returned[chunk].reshape(total_rows, piece_width)
        parts = lax.dot_general(
            mix, back, (((0,), (0,)), ((), ())), preferred_element_type=jnp.float32
        )
        half = folds * token_count
        summed = parts[:half] + parts[half:]
        for fold in range(folds):
            routed_pieces.append(summed[fold * token_count : (fold + 1) * token_count])
    routed = jnp.concatenate(routed_pieces, axis=1)
    layer_out = normalize_rows(
        resid_scale * hidden.astype(jnp.float32) + routed, final_gain
    ).astype(jnp.bfloat16)
    return layer_out[None]


def solution(mesh):
    in_specs = (
        P("dp", "sp", None),
        P("dp", "sp", None),
        P("dp", "sp", None),
        P("dp", "sp", None),
        P("dp", "sp", None),
        P(None, "dp"),
        P(),
        P("dp", "sp", None),
        P("dp", "sp", None),
        P(("sp", "dp"), None, None),
        P(("sp", "dp"), None, None),
        P(("sp", "dp"), None, None),
        P(),
    )
    out_specs = P("dp", "sp", None)
    return jax.shard_map(
        per_device, mesh=mesh, in_specs=in_specs, out_specs=out_specs, check_vma=False
    )
```
